256 devices in a mesh: sp: 16 (over y, x), tp: 16 (over z, core).
Axes of the slice: x: 4, y: 4, z: 8, core: 2. Of those that a mesh axis runs over, the one named last changes fastest.
Arguments:
- conv_in: bfloat16 [1024, 65536], P('tp', 'sp'), may hold values from -6 to 6
- in_gate: bfloat16 [1024, 65536], P('tp', 'sp'), may hold values from -6 to 6
- out_gate: bfloat16 [1024, 65536], P('tp', 'sp'), may hold values from -6 to 6
- doc_ids: int32 [65536], P('sp'), may hold values from 0 to 7, never falling along the last dimension, each value on 1 to 12288 neighbouring positions
- conv_taps: float32 [1024, 3], P('tp'), may hold values from -3.5 to 3.5
- head_gain: float32 [1024], P('tp'), may hold values from 0.1 to 1.9
- out_proj: bfloat16 [1024, 2048], P('tp'), may hold values from -0.1875 to 0.1875
- resid: bfloat16 [65536, 2048], P(('sp', 'tp')), may hold values from -6 to 6
- norm_gain: float32 [2048], replicated, may hold values from 0.1 to 1.9
- route_ids: int32 [65536, 2], P(('sp', 'tp')), may hold values from 0 to 15, all different within a row; in each aligned block of 128 rows (0 to 127, 128 to 255, ...) at most 32 rows name the same one
- route_weight: float32 [65536, 2], P(('sp', 'tp')), may hold values from 0.1 to 1
- w_gate: bfloat16 [16, 2048, 512], P('sp'), may hold values from -0.125 to 0.125
- w_up: bfloat16 [16, 2048, 512], P('sp'), may hold values from -0.125 to 0.125
- w_down: bfloat16 [16, 512, 2048], P('sp'), may hold values from -0.25 to 0.25
Outputs:
- layer_out: bfloat16 [65536, 2048], P(('sp', 'tp'))
The draws below stay inside these ranges and needn't reach their ends.
Inputs may be any that keep to these rules, and one draw needn't show every extreme that they name: `doc_ids`: document numbers never fall along the sequence; every number from 0 to 7 is used; no document is longer than 12288 positions and one is exactly that long. `route_ids`: each position names 2 different experts. In every aligned block of 128 positions no expert is named by more than 32 positions, a bound that some block reaches.
All inputs are finite; a program needn't handle non-finite values.
Results may differ from the reference program's by a relative error of at most 0.0051.
Values may be sent and summed in bfloat16 or wider, within the bound.
A program may use at most 64 MiB of HBM per device.

```python
import math
import jax
import jax.numpy as jnp
import numpy as np
from jax import lax

D = 2048
HEAD = 64
CONV_CH = 1024
EXPERTS = 16
FF = 512
TOPK = 2
TOK_DEV = 4096
SEQ = 65536
HALF = 128
SLOT = 32
DOCS = 8


def level_of(own_key, dims, split, least, high):
    loudness, own = 1.0, jax.random.fold_in(own_key, 6)
    for axis_at, parts in split:
        draws = jnp.exp(jax.random.uniform(jax.random.fold_in(own, axis_at), (parts,), jnp.float32, least / len(split), high / len(split)))
        loudness = loudness * jnp.repeat(draws, dims[axis_at] // parts).reshape([-1 if axis == axis_at else 1 for axis in range(len(dims))])
    return loudness


def profile(number_of, total, most, skew):
    loads = [(1 << 20) // math.isqrt(grade ** skew) + 1 for grade in range(2, number_of + 1)]
    rest, given = total - most - (number_of - 1), [1] * (number_of - 1)
    while rest > 0:
        candidates = [i for i in range(number_of - 1) if given[i] < most]
        pool, left = sum([loads[i] for i in candidates]), rest
        for i in candidates:
            more = min(most - given[i], max(1, left * loads[i] // pool), rest)
            given[i] = given[i] + more
            rest = rest - more
    return np.array([most] + given)


def ragged_sizes(own_key, count, total, bound, lean):
    if count == 2:
        one = jax.random.randint(own_key, (), max(1, total - bound), min(bound, total - 1) + 1)
        return jnp.stack([one, total - one])
    sizes = jnp.asarray(profile(count, total, bound, lean), jnp.int32)
    twos = (count - 1) // 2
    source_of, receiver = sizes[1:1 + 2 * twos:2], sizes[2:2 + 2 * twos:2]
    room = jnp.minimum(source_of - 1, bound - receiver)
    passed = jax.random.randint(jax.random.fold_in(own_key, 1), (twos,), 0, 1 << 20) % (room + 1)
    sizes = sizes.at[1:1 + 2 * twos:2].set(source_of - passed).at[2:2 + 2 * twos:2].set(receiver + passed)
    return sizes[jax.random.permutation(jax.random.fold_in(own_key, 2), count)]


def assign_block(own_key, own, number, rows, number_of, top, limit, skew):
    ranking = jax.random.permutation(own_key, number_of)
    packed, common = load_shares(number_of, rows * top, limit, skew, True), load_shares(number_of, rows * top, limit, skew, False)
    places = jnp.arange(number_of)

    def named(lengths, offset_by):
        used = int((lengths > 0).sum())
        fixed = max(1, used // 4)
        shifted = fixed + (places - fixed + offset_by * (used - fixed)) % max(1, number_of - fixed)
        return jnp.zeros((number_of,), jnp.int32).at[ranking[jnp.where(places < fixed, places, shifted)]].set(jnp.asarray(lengths, jnp.int32))

    lengths = jnp.where(number % 4 == 0, named(packed, number // 4), named(common, number - number // 4 - 1))
    mixed = jax.random.permutation(jax.random.fold_in(own, 3), number_of)
    source_of, receiver = mixed[0:number_of // 2 * 2:2], mixed[1:number_of // 2 * 2:2]
    slack = jnp.minimum(lengths[source_of] - 1, limit - lengths[receiver]) // 2
    slack = jnp.where((source_of == ranking[0]) | (receiver == ranking[0]) | (lengths[receiver] == 0), 0, jnp.maximum(slack, 0))
    shifted = jax.random.randint(jax.random.fold_in(own, 4), (number_of // 2,), 0, 1 << 20) % (slack + 1)
    lengths = lengths.at[source_of].add(-shifted).at[receiver].add(shifted)
    members = jnp.searchsorted(jnp.cumsum(lengths), jnp.arange(rows * top), side="right").astype(jnp.int32)
    listing = members.reshape(top, rows).T
    listing = listing[jax.random.permutation(jax.random.fold_in(own, 1), rows)]
    offset_by = jax.random.randint(jax.random.fold_in(own, 2), (rows, 1), 0, top)
    return jnp.take_along_axis(listing, (jnp.arange(top)[None, :] + offset_by) % top, axis=1)


def load_shares(number_of, total, reach, skew, full):
    weights = [(1 << 20) // math.isqrt(rank ** skew) + 1 for rank in range(1, number_of + 1)]
    largest = reach if full else min(reach, max(-(-total // number_of), total * weights[0] // sum(weights)))
    least = 1 if total - largest >= number_of - 1 else 0
    counts, rest = [largest] + [least] * (number_of - 1), total - largest - least * (number_of - 1)
    while rest > 0:
        movable = [i for i in range(1, number_of) if counts[i] < largest] or [i for i in range(1, number_of) if counts[i] < reach]
        mass, budget = sum([weights[i] for i in movable]), rest
        for i in movable:
            extra = min(reach - counts[i], max(1, budget * weights[i] // mass), rest)
            counts[i] = counts[i] + extra
            rest = rest - extra
    return np.array(counts)


def centred(stream_key, extent, scale, limit, shards=(), held_as=jnp.bfloat16):
    factor_of = level_of(stream_key, extent, shards, -0.22, 0.18) if shards else 1.0
    values = jax.random.normal(stream_key, extent, jnp.float32) * scale * factor_of
    return jnp.minimum(jnp.maximum(values, -limit), limit).astype(held_as)


def setup_inputs(seed: int = 0) -> dict:
    key_of = jax.random.split(jax.random.key(seed), 15)
    conv_in = centred(key_of[0], (CONV_CH, SEQ), 1.0, 6.0, ((0, 16), (1, 16)))
    in_gate = centred(key_of[1], (CONV_CH, SEQ), 1.0, 6.0, ((0, 16), (1, 16)))
    out_gate = centred(key_of[2], (CONV_CH, SEQ), 1.0, 6.0, ((0, 16), (1, 16)))
    doc_ids = jnp.searchsorted(jnp.cumsum(ragged_sizes(key_of[3], DOCS, SEQ, 3 * TOK_DEV, 0)), jnp.arange(SEQ), side="right").astype(jnp.int32)
    conv_taps = centred(key_of[4], (CONV_CH, 3), 3 ** -0.5, 3.5, ((0, 16),), jnp.float32)
    head_gain = jnp.clip(1.0 + 0.18 * jax.random.normal(key_of[5], (CONV_CH,), jnp.float32), 0.1, 1.9)
    out_proj = centred(key_of[6], (CONV_CH, D), CONV_CH ** -0.5, 0.1875, ((0, 16),))
    resid = centred(key_of[7], (SEQ, D), 1.0, 6.0, ((0, 256),))
    norm_gain = jnp.clip(1.0 + 0.18 * jax.random.normal(key_of[8], (D,), jnp.float32), 0.1, 1.9)
    route_ids_keys = jax.random.split(jax.random.fold_in(key_of[9], 1), SEQ // HALF)
    route_ids_turns = jax.random.permutation(jax.random.fold_in(key_of[9], 3), SEQ // HALF)
    route_ids = jax.vmap(lambda own, number: assign_block(jax.random.fold_in(key_of[9], 2), own, number, HALF, EXPERTS, TOPK, SLOT, 1))(route_ids_keys, route_ids_turns).reshape((SEQ, TOPK))
    route_weight = jnp.clip(0.1 + 0.9 * jax.random.uniform(key_of[10], (SEQ, TOPK), jnp.float32) ** level_of(key_of[10], (SEQ, TOPK), ((0, 256),), -0.2, 0.2), 0.1, 1.0)
    w_gate = centred(key_of[11], (EXPERTS, D, FF), D ** -0.5, 0.125, ((0, 16),))
    w_up = centred(key_of[12], (EXPERTS, D, FF), D ** -0.5, 0.125, ((0, 16),))
    w_down = centred(key_of[13], (EXPERTS, FF, D), FF ** -0.5, 0.25, ((0, 16),))
    return {"conv_in": conv_in, "in_gate": in_gate, "out_gate": out_gate, "doc_ids": doc_ids, "conv_taps": conv_taps, "head_gain": head_gain, "out_proj": out_proj, "resid": resid, "norm_gain": norm_gain, "route_ids": route_ids, "route_weight": route_weight, "w_gate": w_gate, "w_up": w_up, "w_down": w_down}


norm_eps = 1e-06

def reference(conv_in, in_gate, out_gate, doc_ids, conv_taps, head_gain, out_proj, resid, norm_gain, route_ids, route_weight, w_gate, w_up, w_down):
    gated_in = in_gate.astype(jnp.float32) * conv_in.astype(jnp.float32)
    channels = gated_in.shape[0]
    earlier = jnp.concatenate([jnp.full((2,), -1, jnp.int32), doc_ids.astype(jnp.int32)])
    same_one = (earlier[1:-1] == doc_ids).astype(jnp.float32)
    same_two = (earlier[:-2] == doc_ids).astype(jnp.float32)
    padded = jnp.concatenate([jnp.zeros((channels, 2), jnp.float32), gated_in], axis=1)
    conv_out = conv_taps[:, 2:3] * gated_in + conv_taps[:, 1:2] * (padded[:, 1:-1] * same_one) + conv_taps[:, 0:1] * (padded[:, :-2] * same_two)
    gated_out = out_gate.astype(jnp.float32) * conv_out
    by_head = gated_out.reshape(channels // HEAD, HEAD, -1)
    by_head = by_head * lax.rsqrt(lax.optimization_barrier(jnp.mean(by_head * by_head, axis=1, keepdims=True)) + norm_eps)
    head_normed = (by_head.reshape(channels, -1) * head_gain[:, None]).astype(jnp.bfloat16)
    mixed = jnp.dot(head_normed.astype(jnp.float32).T, out_proj.astype(jnp.float32))
    stream = resid.astype(jnp.float32) + mixed
    expert_in = (stream * lax.rsqrt(lax.optimization_barrier(jnp.mean(stream * stream, axis=1, keepdims=True)) + norm_eps) * norm_gain).astype(jnp.bfloat16)
    flat_ids = route_ids.reshape(-1).astype(jnp.int32)
    flat_tok = (jnp.arange(flat_ids.shape[0], dtype=jnp.int32) // TOPK).astype(jnp.int32)
    flat_weight = route_weight.reshape(-1)
    most_rows = min(SEQ, SLOT * (SEQ // HALF))

    def one_expert(totals, inputs):
        gate_mat, up_mat, down_mat, number = inputs
        ranked = jnp.argsort((flat_ids != number).astype(jnp.int32), stable=True)[:most_rows]
        picked = flat_tok[ranked]
        weight = jnp.where(flat_ids[ranked] == number, flat_weight[ranked], jnp.zeros_like(flat_weight[ranked]))
        sel_rows = expert_in[picked].astype(jnp.float32)
        gate_part = jnp.dot(sel_rows, gate_mat.astype(jnp.float32))
        up_part = jnp.dot(sel_rows, up_mat.astype(jnp.float32))
        hidden = (jax.nn.silu(gate_part) * up_part).astype(jnp.bfloat16)
        expert_out = jnp.dot(hidden.astype(jnp.float32), down_mat.astype(jnp.float32)).astype(jnp.bfloat16)
        return (totals.at[picked].add(expert_out.astype(jnp.float32) * weight[:, None]), None)
    totals, _ = lax.scan(one_expert, jnp.zeros(stream.shape, jnp.float32), (w_gate, w_up, w_down, jnp.arange(EXPERTS, dtype=jnp.int32)))
    return (stream + totals).astype(jnp.bfloat16)
```

```python
import jax
import jax.numpy as jnp
from jax import lax
from jax.experimental import pallas as pl
from jax.experimental.pallas import tpu as pltpu
from jax.sharding import Mesh
from jax.sharding import PartitionSpec as P

HEAD = 64
TP = ("tp_0", "tp_1")
SP_TP = ("sp", "tp_0", "tp_1")
SIDE = 4
PARTNERS = SIDE * SIDE
BLOCKS = 2


norm_eps = 1e-06


def shifted(value, axis, steps):
    count = lax.axis_size(axis)
    leading, last = (max(0, -steps), min(count, count - steps))
    return lax.ppermute(value, axis, [(source, source + steps) for source in range(leading, last)])


def cut_along(array, dim, length):
    before, after = (array.shape[:dim], array.shape[dim + 1 :])
    return jnp.moveaxis(array.reshape(*before, length, -1, *after), dim, 0)


def joined_along(pieces, dim):
    dims = list(pieces.shape[1:])
    dims[dim] *= pieces.shape[0]
    return jnp.moveaxis(pieces, 0, dim).reshape(dims)


def exchange_in_order(pieces, axes, sequence):
    dims = [lax.axis_size(a) for a in axes]
    pieces = pieces.reshape(*dims, *pieces.shape[1:])
    for k in sequence:
        pieces = lax.all_to_all(pieces, axes[k], split_axis=k, concat_axis=k, tiled=True)
    return pieces.reshape(-1, *pieces.shape[len(axes) :])


def exchange_by_chip(array, groups, sequence, split_dim, concat_dim):
    length = lax.axis_size(groups[0]) * lax.axis_size(groups[1])
    pieces = cut_along(array, split_dim, length)
    return joined_along(exchange_in_order(pieces, groups, sequence), concat_dim)


def core_index():
    return lax.axis_index("tp_1")


def partner(first, second):
    me, core = lax.axis_index("sp"), core_index()
    step_y = core * first + (1 - core) * second
    step_x = (1 - core) * first + core * second
    y = ((me >> 2) + step_y) & (SIDE - 1)
    x = ((me & (SIDE - 1)) + step_x) & (SIDE - 1)
    return {"sp": y * SIDE + x}


def copies_to(sources, targets, send, recv, partners):
    return [
        pltpu.make_async_remote_copy(
            source, target, send.at[i], recv.at[i],
            device_id=device, device_id_type=pl.DeviceIdType.MESH,
        )
        for i, (source, target, device) in enumerate(zip(sources, targets, partners))
    ]


def start(copies):
    for copy in copies:
        copy.start()


def arrived(copies):
    for copy in copies:
        copy.wait_recv()


def experts_kernel(
    rows_ref, table_ref, weight_hi, weight_lo, stream_ref, gate_hbm, up_hbm, down_hbm,
    out_ref,
    send_buf, there, answers, back_buf, gate_ref, up_ref, down_ref, load_sems, own_sems,
    *sems,
):
    loads = [
        pltpu.make_async_copy(hbm, ref, load_sems.at[i])
        for i, (hbm, ref) in enumerate(((gate_hbm, gate_ref), (up_hbm, up_ref), (down_hbm, down_ref)))
    ]
    start(loads)
    others = range(1, SIDE)
    barrier = pltpu.get_barrier_semaphore()
    for step in others:
        for device in (partner(step, 0), partner(0, step)):
            pl.semaphore_signal(
                barrier, inc=1, device_id=device, device_id_type=pl.DeviceIdType.MESH
            )

    half = rows_ref.shape[0] // BLOCKS
    width = rows_ref.shape[1]
    slot = send_buf.shape[3]
    slots = PARTNERS * slot
    cols = 512

    def pack(block):
        @pl.loop(0, width // cols)
        def _(c):
            col = pl.ds(pl.multiple_of(c * cols, cols), cols)
            packed = jnp.dot(
                table_ref[block], rows_ref[pl.ds(block * half, half), col],
                preferred_element_type=jnp.float32,
            ).astype(jnp.bfloat16).reshape(SIDE, SIDE, slot, cols)
            send_buf[block, :, :, :, col] = packed
            there[block, pl.ds(0, SIDE), 0, :, col] = packed[0]

    def experts(block):
        @pl.loop(0, 2)
        def _(m):
            at = pl.ds(SIDE - 1 + m * 2, 2)
            inputs = there[block, at].reshape(slots // 2, width)
            gate = jnp.dot(inputs, gate_ref[...], preferred_element_type=jnp.float32)
            up = jnp.dot(inputs, up_ref[...], preferred_element_type=jnp.float32)
            hidden = (gate / (1.0 + jnp.exp(-gate)) * up).astype(jnp.bfloat16)
            result = jnp.dot(hidden, down_ref[...], preferred_element_type=jnp.float32)
            answers[block, at] = result.astype(jnp.bfloat16).reshape(2, SIDE, slot, width)

    def combine(block):
        @pl.loop(0, width // cols)
        def _(c):
            col = pl.ds(pl.multiple_of(c * cols, cols), cols)
            own = pl.ds(block * half, half)
            back = back_buf[block, :, :, :, col].reshape(slots, cols)
            total = (
                stream_ref[own, col]
                + jnp.dot(weight_hi[block], back, preferred_element_type=jnp.float32)
                + jnp.dot(weight_lo[block], back, preferred_element_type=jnp.float32)
            )
            out_ref[own, col] = total.astype(jnp.bfloat16)

    def ahead(i, b):
        return sems[2 * i].at[b], sems[2 * i + 1].at[b]

    every = pl.ds(0, SIDE)
    out_first = [
        copies_to(
            [send_buf.at[b, f] for f in others], [there.at[b, every, f] for f in others],
            *ahead(0, b), [partner(f, 0) for f in others],
        )
        for b in range(BLOCKS)
    ]
    out_second = [
        copies_to(
            [there.at[b, g - 1] for g in others], [there.at[b, SIDE - 1 + g] for g in others],
            *ahead(1, b), [partner(0, g) for g in others],
        )
        for b in range(BLOCKS)
    ]
    back_second = [
        copies_to(
            [answers.at[b, SIDE - 1 + g] for g in others], [answers.at[b, g - 1] for g in others],
            *ahead(2, b), [partner(0, SIDE - g) for g in others],
        )
        for b in range(BLOCKS)
    ]
    back_first = [
        copies_to(
            [answers.at[b, every, f] for f in others], [back_buf.at[b, f] for f in others],
            *ahead(3, b), [partner(SIDE - f, 0) for f in others],
        )
        for b in range(BLOCKS)
    ]
    own = [
        pltpu.make_async_copy(answers.at[b, every, 0], back_buf.at[b, 0], own_sems.at[b])
        for b in range(BLOCKS)
    ]

    pack(0)
    pl.semaphore_wait(barrier, 2 * (SIDE - 1))
    start(out_first[0])
    pack(1)
    start(out_first[1])
    for b in range(BLOCKS):
        arrived(out_first[b])
        start(out_second[b])
    for load in loads:
        load.wait()
    for b in range(BLOCKS):
        arrived(out_second[b])
        experts(b)
        start(back_second[b])
    for b in range(BLOCKS):
        arrived(back_second[b])
        start(back_first[b])
        own[b].start()
    for b in range(BLOCKS):
        arrived(back_first[b])
        own[b].wait()
        combine(b)
    for copies in (*out_first, *out_second, *back_second, *back_first):
        for copy in copies:
            copy.wait_send()


def experts_call(rows, table, weight_hi, weight_lo, stream, w_gate, w_up, w_down):
    count, width = rows.shape
    slot = table.shape[1] // PARTNERS
    ff = w_gate.shape[1]
    vmem = pl.BlockSpec(memory_space=pltpu.VMEM)
    hbm = pl.BlockSpec(memory_space=pl.ANY)
    square = pltpu.VMEM((BLOCKS, SIDE, SIDE, slot, width), jnp.bfloat16)
    longer = pltpu.VMEM((BLOCKS, 2 * SIDE - 1, SIDE, slot, width), jnp.bfloat16)
    dma = pltpu.SemaphoreType.DMA
    return pl.pallas_call(
        experts_kernel,
        out_shape=jax.ShapeDtypeStruct((count, width), jnp.bfloat16),
        in_specs=[vmem] * 5 + [hbm] * 3,
        out_specs=vmem,
        scratch_shapes=[
            square, longer, longer, square,
            pltpu.VMEM((width, ff), jnp.bfloat16),
            pltpu.VMEM((width, ff), jnp.bfloat16),
            pltpu.VMEM((ff, width), jnp.bfloat16),
            dma((3,)), dma((BLOCKS,)),
            *[dma((BLOCKS, SIDE - 1))] * 8,
        ],
        compiler_params=pltpu.CompilerParams(
            collective_id=1, has_side_effects=True, vmem_limit_bytes=56 * 1024 * 1024
        ),
        name="experts",
    )(rows, table, weight_hi, weight_lo, stream, w_gate, w_up, w_down)


def routing(route_ids, route_weight, slot):
    rows = route_ids.shape[0]
    half = rows // BLOCKS
    me, core = lax.axis_index("sp"), core_index()
    dy = ((route_ids >> 2) - (me >> 2)) & (SIDE - 1)
    dx = (route_ids - me) & (SIDE - 1)
    first = jnp.where(core == 0, dx, dy)
    second = (jnp.where(core == 0, dy, dx) + SIDE - 1) & (SIDE - 1)
    flat = (first * SIDE + second).reshape(BLOCKS, -1)
    order = jnp.arange(flat.shape[1], dtype=jnp.int32)
    same = (flat[:, :, None] == flat[:, None, :]) & (order[:, None] > order[None, :])
    place = (flat * slot + jnp.sum(same.astype(jnp.int32), axis=2)).reshape(BLOCKS, half, -1)
    targets = jnp.arange(PARTNERS * slot, dtype=jnp.int32)
    table = jnp.any(targets[None, :, None, None] == place[:, None], axis=3).astype(jnp.bfloat16)
    hit = (place[:, :, :, None] == targets).astype(jnp.float32)
    weight = jnp.sum(hit * route_weight.reshape(BLOCKS, half, -1, 1), axis=2)
    weight_hi = weight.astype(jnp.bfloat16)
    weight_lo = (weight - weight_hi.astype(jnp.float32)).astype(jnp.bfloat16)
    return table, weight_hi, weight_lo


def body(
    conv_in,
    in_gate,
    out_gate,
    doc_ids,
    conv_taps,
    head_gain,
    out_proj,
    resid,
    norm_gain,
    route_ids,
    route_weight,
    w_gate,
    w_up,
    w_down,
):
    gated_in = in_gate.astype(jnp.float32) * conv_in.astype(jnp.float32)
    doc_value = doc_ids.astype(jnp.float32)
    earlier_in, earlier_doc = shifted((gated_in[:, -2:], doc_value[-2:]), "sp", 1)
    padded_in = jnp.concatenate([earlier_in, gated_in], axis=1)
    padded_doc = jnp.concatenate([earlier_doc, doc_value])
    same_one = (padded_doc[1:-1] == doc_value).astype(jnp.float32)
    same_two = (padded_doc[:-2] == doc_value).astype(jnp.float32)
    conv_out = (
        conv_taps[:, 2:3] * gated_in
        + conv_taps[:, 1:2] * (padded_in[:, 1:-1] * same_one)
        + conv_taps[:, 0:1] * (padded_in[:, :-2] * same_two)
    )
    gated_out = out_gate.astype(jnp.float32) * conv_out
    channels = gated_out.shape[0]
    by_head = gated_out.reshape(channels // HEAD, HEAD, -1)
    by_head = by_head * lax.rsqrt(jnp.mean(by_head * by_head, axis=1, keepdims=True) + norm_eps)
    head_normed = (by_head.reshape(channels, -1) * head_gain[:, None]).astype(jnp.bfloat16)
    by_row = exchange_by_chip(head_normed, ("tp_0", "tp_1"), (0, 1), 1, 0)
    rows = resid.shape[0]
    mixed = lax.dot_general(
        by_row,
        lax.all_gather(out_proj, TP, axis=0, tiled=True),
        (((0,), (0,)), ((), ())),
        preferred_element_type=jnp.float32,
    )
    stream = resid.astype(jnp.float32) + mixed
    expert_in = (
        stream * lax.rsqrt(jnp.mean(stream * stream, axis=1, keepdims=True) + norm_eps) * norm_gain
    ).astype(jnp.bfloat16)
    slot = max(2, rows // 8)
    table, weight_hi, weight_lo = routing(route_ids, route_weight, slot)
    return experts_call(
        expert_in, table, weight_hi, weight_lo, stream, w_gate[0], w_up[0], w_down[0]
    )


def solution(mesh):
    finer = Mesh(mesh.devices.reshape(mesh.shape["sp"], 8, 2), ("sp", "tp_0", "tp_1"))
    return jax.shard_map(
        body,
        mesh=finer,
        in_specs=(
            P(TP, "sp"),
            P(TP, "sp"),
            P(TP, "sp"),
            P("sp"),
            P(TP, None),
            P(TP),
            P(TP, None),
            P(SP_TP, None),
            P(),
            P(SP_TP, None),
            P(SP_TP, None),
            P("sp", None, None),
            P("sp", None, None),
            P("sp", None, None),
        ),
        out_specs=P(SP_TP, None),
        check_vma=False,
    )
```

```python
import jax
import jax.numpy as jnp
from jax import lax
from jax.experimental import pallas as pl
from jax.experimental.pallas import tpu as pltpu
from jax.sharding import Mesh
from jax.sharding import PartitionSpec as P

HEAD = 64
TP = ("tp_0", "tp_1")
LANES = 128
HALO = LANES
SP_TP = ("sp", "tp_0", "tp_1")
SIDE = 4
PARTNERS = SIDE * SIDE
BLOCKS = 2


norm_eps = 1e-06


def core_index():
    return lax.axis_index("tp_1")


def place_at(core, first, second):
    me = lax.axis_index("sp")
    step_y = core * first + (1 - core) * second
    step_x = (1 - core) * first + core * second
    y = ((me >> 2) + step_y) & (SIDE - 1)
    x = ((me & (SIDE - 1)) + step_x) & (SIDE - 1)
    return y * SIDE + x


def partner(first, second):
    return {"sp": place_at(core_index(), first, second)}


def tp_partner(steps):
    depth = lax.axis_size("tp_0")
    tp = (lax.axis_index("tp_0") * 2 + core_index() + steps) & (2 * depth - 1)
    return {"tp_0": tp >> 1, "tp_1": tp & 1}


def next_block(steps):
    return {"sp": (lax.axis_index("sp") + steps) & (PARTNERS - 1)}


def remote(source, target, send, recv, device):
    return pltpu.make_async_remote_copy(
        source, target, send, recv, device_id=device, device_id_type=pl.DeviceIdType.MESH
    )


def copies_to(sources, targets, send, recv, partners):
    return [
        remote(source, target, send.at[i], recv.at[i], device)
        for i, (source, target, device) in enumerate(zip(sources, targets, partners))
    ]


def start(copies):
    for copy in copies:
        copy.start()


def arrived(copies):
    for copy in copies:
        copy.wait_recv()


def layer_kernel(
    taps_ref, head_ref, norm_ref, table_ref, weight_hi, weight_lo,
    conv_hbm, gate_in_hbm, gate_out_hbm, docs_hbm, proj_hbm, resid_hbm,
    gate_hbm, up_hbm, down_hbm,
    out_ref,
    conv_buf, gate_in_buf, gate_out_buf, docs_buf, resid_buf, normed_buf, by_row, turned,
    proj, rows_ref, stream_ref,
    send_buf, there, answers, back_buf, gate_ref, up_ref, down_ref, load_sems, own_sems,
    halo_send, halo_recv, normed_send, normed_recv,
    deep_send, deep_recv, row_send, row_recv, plane_send, plane_recv, pair_send, pair_recv,
    *sems,
):
    me, core, layer = lax.axis_index("sp"), core_index(), lax.axis_index("tp_0")
    depth = lax.axis_size("tp_0")
    devices = 2 * depth
    channels, length = gate_out_buf.shape
    chunk = length // devices
    others = range(1, SIDE)
    barrier = pltpu.get_barrier_semaphore()
    greeted = [partner(step, 0) for step in others] + [partner(0, step) for step in others]
    greeted += [next_block(1), next_block(-1)] + [tp_partner(k) for k in range(1, devices)]
    for device in greeted:
        pl.semaphore_signal(barrier, inc=1, device_id=device, device_id_type=pl.DeviceIdType.MESH)

    body_at, halo_at = pl.ds(HALO, length), pl.ds(0, HALO)
    tail_at = pl.ds(length, HALO)
    own_shard = pl.ds(pl.multiple_of(layer * channels, channels), channels)
    own_cols = pl.ds(pl.multiple_of(me * LANES, LANES), LANES)
    pairs = (
        (proj_hbm.at[:, own_cols], proj.at[core, me, own_shard]),
        (conv_hbm, conv_buf.at[:, body_at]),
        (gate_in_hbm, gate_in_buf.at[:, body_at]),
        (docs_hbm, docs_buf.at[:, body_at]),
        (gate_out_hbm, gate_out_buf),
        (resid_hbm, resid_buf),
        (gate_hbm, gate_ref),
        (up_hbm, up_ref),
        (down_hbm, down_ref),
    )
    loads = [
        pltpu.make_async_copy(source, target, load_sems.at[i])
        for i, (source, target) in enumerate(pairs)
    ]
    start(loads)
    halo = [
        remote(buf.at[:, tail_at], buf.at[:, halo_at], halo_send.at[i], halo_recv.at[i], next_block(1))
        for i, buf in enumerate((conv_buf, gate_in_buf, docs_buf))
    ]
    deep = [
        remote(
            proj.at[core, me, own_shard], proj.at[core, me, own_shard],
            deep_send.at[k - 1], deep_recv.at[k - 1], tp_partner(2 * k),
        )
        for k in range(1, depth)
    ]
    pl.semaphore_wait(barrier, len(greeted))
    loads[0].wait()
    start(deep)
    for load in loads[1:4]:
        load.wait()
    start(halo)
    loads[4].wait()

    def normed_copy(k):
        to = pl.multiple_of((core * depth + layer) * channels, channels)
        return remote(
            normed_buf.at[k], by_row.at[pl.ds(to, channels)], normed_send.at[k], normed_recv.at[k],
            tp_partner(k),
        )

    def convolved(k):
        j = (layer * 2 + core + k) & (devices - 1)

        @pl.when(j == 0)
        def _():
            arrived(halo)

        wide = pl.ds(pl.multiple_of(j * chunk, chunk), chunk + HALO)
        gated = conv_buf[:, wide].astype(jnp.float32) * gate_in_buf[:, wide].astype(jnp.float32)
        docs = jnp.broadcast_to(docs_buf[:, wide], (8, chunk + HALO))
        lane = lax.broadcasted_iota(jnp.int32, docs.shape, 1)
        docs = jnp.where((j == 0) & (me == 0) & (lane < HALO), -1, docs)
        same_one = (pltpu.roll(docs, 1, 1) == docs).astype(jnp.float32)[:1, HALO:]
        same_two = (pltpu.roll(docs, 2, 1) == docs).astype(jnp.float32)[:1, HALO:]
        conv = (
            taps_ref[:, 2:3] * gated[:, HALO:]
            + taps_ref[:, 1:2] * (pltpu.roll(gated, 1, 1)[:, HALO:] * same_one)
            + taps_ref[:, 0:1] * (pltpu.roll(gated, 2, 1)[:, HALO:] * same_two)
        )
        own = pl.ds(pl.multiple_of(j * chunk, chunk), chunk)
        value = gate_out_buf[:, own].astype(jnp.float32) * conv
        scale = lax.rsqrt(jnp.mean(value * value, axis=0, keepdims=True) + norm_eps)
        return (value * scale * head_ref[...]).astype(jnp.bfloat16)

    @pl.loop(0, devices - 1)
    def _(i):
        k = devices // 2 + jnp.where((i & 1) == 1, -((i + 1) >> 1), i >> 1)
        normed_buf[k] = convolved(k)
        normed_copy(k).start()

    by_row[pl.ds(pl.multiple_of((core * depth + layer) * channels, channels), channels)] = convolved(0)

    def piece(f, g, c=core):
        return proj.at[c, place_at(c, f, g)]

    def pair_copy(f, g, c):
        return remote(
            piece(f, g, c), piece(f, g, c),
            pair_send.at[f & (SIDE - 1), g & (SIDE - 1)], pair_recv.at[f & (SIDE - 1), g & (SIDE - 1)],
            {"tp_1": 1 - core},
        )

    row = [
        remote(piece(0, 0), piece(0, 0), row_send.at[f - 1], row_recv.at[f - 1], partner(f, 0))
        for f in others
    ]
    plane = {
        (f, g): remote(
            piece(-f, 0), piece(-f, 0), plane_send.at[f, g - 1], plane_recv.at[f, g - 1], partner(0, g)
        )
        for f in range(SIDE) for g in others
    }
    arrived(deep)
    start(row)
    start([plane[0, g] for g in others])
    pair_copy(0, 0, core).start()
    for f in (1, 3, 2):
        row[f - 1].wait_recv()
        start([plane[f, g] for g in others])
        pair_copy(-f, 0, core).start()

    for k in range(1, devices):
        normed_copy(k).wait_recv()
    turned[...] = by_row[...].T
    for g in (1, 3, 2):
        for f in range(SIDE):
            plane[f, g].wait_recv()
            pair_copy(-f, -g, core).start()
    for f in range(SIDE):
        for g in range(SIDE):
            pair_copy(-f, -g, 1 - core).wait_recv()
    loads[5].wait()

    count = resid_buf.shape[0]
    step = 2

    def project(i, total):
        col = pl.ds(pl.multiple_of(i * step * LANES, step * LANES), step * LANES)
        mixed = jnp.zeros((count, step * LANES), jnp.float32)
        for c in range(2):
            right = jnp.concatenate([proj[c, i * step + n] for n in range(step)], axis=1)
            left = turned[:, pl.ds(c * depth * channels, depth * channels)]
            mixed = mixed + jnp.dot(left, right, preferred_element_type=jnp.float32)
        value = resid_buf[:, col].astype(jnp.float32) + mixed
        stream_ref[:, col] = value
        return total + value * value

    total = lax.fori_loop(
        0, PARTNERS // step, project, jnp.zeros((count, step * LANES), jnp.float32)
    )
    mean = jnp.sum(total, axis=1, keepdims=True) / (PARTNERS * LANES)
    scale = lax.rsqrt(mean + norm_eps)

    @pl.loop(0, PARTNERS // step)
    def _(i):
        col = pl.ds(pl.multiple_of(i * step * LANES, step * LANES), step * LANES)
        rows_ref[:, col] = (stream_ref[:, col] * scale * norm_ref[:, col]).astype(jnp.bfloat16)

    half = rows_ref.shape[0] // BLOCKS
    width = rows_ref.shape[1]
    slot = send_buf.shape[3]
    slots = PARTNERS * slot
    cols = 512

    def pack(block):
        @pl.loop(0, width // cols)
        def _(c):
            col = pl.ds(pl.multiple_of(c * cols, cols), cols)
            packed = jnp.dot(
                table_ref[block], rows_ref[pl.ds(block * half, half), col],
                preferred_element_type=jnp.float32,
            ).astype(jnp.bfloat16).reshape(SIDE, SIDE, slot, cols)
            send_buf[block, :, :, :, col] = packed
            there[block, pl.ds(0, SIDE), 0, :, col] = packed[0]

    def experts(block):
        @pl.loop(0, 2)
        def _(m):
            at = pl.ds(SIDE - 1 + m * 2, 2)
            inputs = there[block, at].reshape(slots // 2, width)
            gate = jnp.dot(inputs, gate_ref[...], preferred_element_type=jnp.float32)
            up = jnp.dot(inputs, up_ref[...], preferred_element_type=jnp.float32)
            hidden = (gate / (1.0 + jnp.exp(-gate)) * up).astype(jnp.bfloat16)
            result = jnp.dot(hidden, down_ref[...], preferred_element_type=jnp.float32)
            answers[block, at] = result.astype(jnp.bfloat16).reshape(2, SIDE, slot, width)

    def combine(block):
        @pl.loop(0, width // cols)
        def _(c):
            col = pl.ds(pl.multiple_of(c * cols, cols), cols)
            own = pl.ds(block * half, half)
            back = back_buf[block, :, :, :, col].reshape(slots, cols)
            total = (
                stream_ref[own, col]
                + jnp.dot(weight_hi[block], back, preferred_element_type=jnp.float32)
                + jnp.dot(weight_lo[block], back, preferred_element_type=jnp.float32)
            )
            out_ref[own, col] = total.astype(jnp.bfloat16)

    def ahead(i, b):
        return sems[2 * i].at[b], sems[2 * i + 1].at[b]

    every = pl.ds(0, SIDE)
    out_first = [
        copies_to(
            [send_buf.at[b, f] for f in others], [there.at[b, every, f] for f in others],
            *ahead(0, b), [partner(f, 0) for f in others],
        )
        for b in range(BLOCKS)
    ]
    out_second = [
        copies_to(
            [there.at[b, g - 1] for g in others], [there.at[b, SIDE - 1 + g] for g in others],
            *ahead(1, b), [partner(0, g) for g in others],
        )
        for b in range(BLOCKS)
    ]
    back_second = [
        copies_to(
            [answers.at[b, SIDE - 1 + g] for g in others], [answers.at[b, g - 1] for g in others],
            *ahead(2, b), [partner(0, SIDE - g) for g in others],
        )
        for b in range(BLOCKS)
    ]
    back_first = [
        copies_to(
            [answers.at[b, every, f] for f in others], [back_buf.at[b, f] for f in others],
            *ahead(3, b), [partner(SIDE - f, 0) for f in others],
        )
        for b in range(BLOCKS)
    ]
    own = [
        pltpu.make_async_copy(answers.at[b, every, 0], back_buf.at[b, 0], own_sems.at[b])
        for b in range(BLOCKS)
    ]

    pack(0)
    start(out_first[0])
    pack(1)
    start(out_first[1])
    for b in range(BLOCKS):
        arrived(out_first[b])
        start(out_second[b])
    for load in loads[6:]:
        load.wait()
    for b in range(BLOCKS):
        arrived(out_second[b])
        experts(b)
        start(back_second[b])
    for b in range(BLOCKS):
        arrived(back_second[b])
        start(back_first[b])
        own[b].start()
    for b in range(BLOCKS):
        arrived(back_first[b])
        own[b].wait()
        combine(b)
    sent = [*halo, *deep, *row, *plane.values(), *[normed_copy(k) for k in range(1, devices)]]
    sent += [pair_copy(-f, -g, core) for f in range(SIDE) for g in range(SIDE)]
    for copies in (sent, *out_first, *out_second, *back_second, *back_first):
        for copy in copies:
            copy.wait_send()


def layer_call(
    conv_in, in_gate, out_gate, docs, taps, head_gain, out_proj, resid, norm_gain,
    table, weight_hi, weight_lo, w_gate, w_up, w_down,
):
    count, width = resid.shape
    channels, length = conv_in.shape
    slot = table.shape[1] // PARTNERS
    ff = w_gate.shape[1]
    depth = lax.axis_size("tp_0")
    devices = 2 * depth
    bf16 = jnp.bfloat16
    vmem = pl.BlockSpec(memory_space=pltpu.VMEM)
    hbm = pl.BlockSpec(memory_space=pl.ANY)
    square = pltpu.VMEM((BLOCKS, SIDE, SIDE, slot, width), bf16)
    longer = pltpu.VMEM((BLOCKS, 2 * SIDE - 1, SIDE, slot, width), bf16)
    dma = pltpu.SemaphoreType.DMA
    return pl.pallas_call(
        layer_kernel,
        out_shape=jax.ShapeDtypeStruct((count, width), bf16),
        in_specs=[vmem] * 6 + [hbm] * 9,
        out_specs=vmem,
        scratch_shapes=[
            pltpu.VMEM((channels, HALO + length), bf16),
            pltpu.VMEM((channels, HALO + length), bf16),
            pltpu.VMEM((channels, length), bf16),
            pltpu.VMEM((1, HALO + length), jnp.int32),
            pltpu.VMEM((count, width), bf16),
            pltpu.VMEM((devices, channels, length // devices), bf16),
            pltpu.VMEM((devices * channels, count), bf16),
            pltpu.VMEM((count, devices * channels), bf16),
            pltpu.VMEM((2, PARTNERS, depth * channels, width // PARTNERS), bf16),
            pltpu.VMEM((count, width), bf16),
            pltpu.VMEM((count, width), jnp.float32),
            square, longer, longer, square,
            pltpu.VMEM((width, ff), bf16),
            pltpu.VMEM((width, ff), bf16),
            pltpu.VMEM((ff, width), bf16),
            dma((9,)), dma((BLOCKS,)),
            dma((3,)), dma((3,)), dma((devices,)), dma((devices,)),
            dma((depth - 1,)), dma((depth - 1,)), dma((SIDE - 1,)), dma((SIDE - 1,)),
            dma((SIDE, SIDE - 1)), dma((SIDE, SIDE - 1)), dma((SIDE, SIDE)), dma((SIDE, SIDE)),
            *[dma((BLOCKS, SIDE - 1))] * 8,
        ],
        compiler_params=pltpu.CompilerParams(
            collective_id=1, has_side_effects=True, vmem_limit_bytes=60 * 1024 * 1024
        ),
        name="layer",
    )(
        taps, head_gain, norm_gain, table, weight_hi, weight_lo,
        conv_in, in_gate, out_gate, docs, out_proj, resid, w_gate, w_up, w_down,
    )


def routing(route_ids, route_weight, slot):
    rows = route_ids.shape[0]
    half = rows // BLOCKS
    me, core = lax.axis_index("sp"), core_index()
    dy = ((route_ids >> 2) - (me >> 2)) & (SIDE - 1)
    dx = (route_ids - me) & (SIDE - 1)
    first = jnp.where(core == 0, dx, dy)
    second = (jnp.where(core == 0, dy, dx) + SIDE - 1) & (SIDE - 1)
    flat = (first * SIDE + second).reshape(BLOCKS, -1)
    order = jnp.arange(flat.shape[1], dtype=jnp.int32)
    same = (flat[:, :, None] == flat[:, None, :]) & (order[:, None] > order[None, :])
    place = (flat * slot + jnp.sum(same.astype(jnp.int32), axis=2)).reshape(BLOCKS, half, -1)
    targets = jnp.arange(PARTNERS * slot, dtype=jnp.int32)
    table = jnp.any(targets[None, :, None, None] == place[:, None], axis=3).astype(jnp.bfloat16)
    hit = (place[:, :, :, None] == targets).astype(jnp.float32)
    weight = jnp.sum(hit * route_weight.reshape(BLOCKS, half, -1, 1), axis=2)
    weight_hi = weight.astype(jnp.bfloat16)
    weight_lo = (weight - weight_hi.astype(jnp.float32)).astype(jnp.bfloat16)
    return table, weight_hi, weight_lo


def body(
    conv_in,
    in_gate,
    out_gate,
    doc_ids,
    conv_taps,
    head_gain,
    out_proj,
    resid,
    norm_gain,
    route_ids,
    route_weight,
    w_gate,
    w_up,
    w_down,
):
    slot = max(2, resid.shape[0] // 8)
    table, weight_hi, weight_lo = routing(route_ids, route_weight, slot)
    return layer_call(
        conv_in, in_gate, out_gate, doc_ids.reshape(1, -1), conv_taps, head_gain.reshape(-1, 1),
        out_proj, resid, norm_gain.reshape(1, -1), table, weight_hi, weight_lo,
        w_gate[0], w_up[0], w_down[0],
    )


def solution(mesh):
    finer = Mesh(mesh.devices.reshape(mesh.shape["sp"], 8, 2), ("sp", "tp_0", "tp_1"))
    return jax.shard_map(
        body,
        mesh=finer,
        in_specs=(
            P(TP, "sp"),
            P(TP, "sp"),
            P(TP, "sp"),
            P("sp"),
            P(TP, None),
            P(TP),
            P(TP, None),
            P(SP_TP, None),
            P(),
            P(SP_TP, None),
            P(SP_TP, None),
            P("sp", None, None),
            P("sp", None, None),
            P("sp", None, None),
        ),
        out_specs=P(SP_TP, None),
        check_vma=False,
    )
```

```python
import jax
import jax.numpy as jnp
from jax import lax
from jax.experimental import pallas as pl
from jax.experimental.pallas import tpu as pltpu
from jax.sharding import Mesh
from jax.sharding import PartitionSpec as P

HEAD = 64
TP = ("tp_0", "tp_1")
LANES = 128
HALO = LANES
SP_TP = ("sp", "tp_0", "tp_1")
SIDE = 4
PARTNERS = SIDE * SIDE
BLOCKS = 2


norm_eps = 1e-06


def core_index():
    return lax.axis_index("tp_1")


def place_at(core, first, second):
    me = lax.axis_index("sp")
    step_y = core * first + (1 - core) * second
    step_x = (1 - core) * first + core * second
    y = ((me >> 2) + step_y) & (SIDE - 1)
    x = ((me & (SIDE - 1)) + step_x) & (SIDE - 1)
    return y * SIDE + x


def partner(first, second):
    return {"sp": place_at(core_index(), first, second)}


def tp_partner(steps):
    depth = lax.axis_size("tp_0")
    tp = (lax.axis_index("tp_0") * 2 + core_index() + steps) & (2 * depth - 1)
    return {"tp_0": tp >> 1, "tp_1": tp & 1}


def next_block(steps):
    return {"sp": (lax.axis_index("sp") + steps) & (PARTNERS - 1)}


def remote(source, target, send, recv, device):
    return pltpu.make_async_remote_copy(
        source, target, send, recv, device_id=device, device_id_type=pl.DeviceIdType.MESH
    )


def copies_to(sources, targets, send, recv, partners):
    return [
        remote(source, target, send.at[i], recv.at[i], device)
        for i, (source, target, device) in enumerate(zip(sources, targets, partners))
    ]


def start(copies):
    for copy in copies:
        copy.start()


def arrived(copies):
    for copy in copies:
        copy.wait_recv()


def layer_kernel(
    taps_ref, head_ref, norm_ref, ids_ref, share_ref,
    conv_hbm, gate_in_hbm, gate_out_hbm, docs_hbm, proj_hbm, resid_hbm,
    gate_hbm, up_hbm, down_hbm,
    out_ref,
    conv_buf, gate_in_buf, gate_out_buf, docs_buf, resid_buf, normed_buf, by_row, turned,
    proj, rows_ref, stream_ref, squares, table_ref, weight_hi, weight_lo,
    send_buf, there, answers, back_buf, gate_ref, up_ref, down_ref, load_sems, own_sems,
    halo_send, halo_recv, normed_send, normed_recv,
    deep_send, deep_recv, row_send, row_recv, plane_send, plane_recv, pair_send, pair_recv,
    *sems,
):
    me, core, layer = lax.axis_index("sp"), core_index(), lax.axis_index("tp_0")
    depth = lax.axis_size("tp_0")
    devices = 2 * depth
    channels, length = gate_out_buf.shape
    chunk = length // devices
    others = range(1, SIDE)
    barrier = pltpu.get_barrier_semaphore()
    greeted = [partner(step, 0) for step in others] + [partner(0, step) for step in others]
    greeted += [next_block(1), next_block(-1)] + [tp_partner(k) for k in range(1, devices)]
    for device in greeted:
        pl.semaphore_signal(barrier, inc=1, device_id=device, device_id_type=pl.DeviceIdType.MESH)

    body_at, halo_at = pl.ds(HALO, length), pl.ds(0, HALO)
    tail_at = pl.ds(length, HALO)
    own_shard = pl.ds(pl.multiple_of(layer * channels, channels), channels)
    own_cols = pl.ds(pl.multiple_of(me * LANES, LANES), LANES)
    pairs = (
        (proj_hbm.at[:, own_cols], proj.at[core, me, own_shard]),
        (conv_hbm, conv_buf.at[:, body_at]),
        (gate_in_hbm, gate_in_buf.at[:, body_at]),
        (docs_hbm, docs_buf.at[:, body_at]),
        (gate_out_hbm, gate_out_buf),
        (resid_hbm, resid_buf),
        (gate_hbm, gate_ref),
        (up_hbm, up_ref),
        (down_hbm, down_ref),
    )
    loads = [
        pltpu.make_async_copy(source, target, load_sems.at[i])
        for i, (source, target) in enumerate(pairs)
    ]
    start(loads)
    halo = [
        remote(buf.at[:, tail_at], buf.at[:, halo_at], halo_send.at[i], halo_recv.at[i], next_block(1))
        for i, buf in enumerate((conv_buf, gate_in_buf, docs_buf))
    ]
    deep = [
        remote(
            proj.at[core, me, own_shard], proj.at[core, me, own_shard],
            deep_send.at[k - 1], deep_recv.at[k - 1], tp_partner(2 * k),
        )
        for k in range(1, depth)
    ]
    def column(row):
        square = (row.shape[1], row.shape[1])
        diagonal = lax.broadcasted_iota(jnp.int32, square, 0) == lax.broadcasted_iota(jnp.int32, square, 1)
        return jnp.sum(jnp.where(diagonal, jnp.broadcast_to(row, square), 0.0), axis=1, keepdims=True)

    def normed_copy(k):
        to = pl.multiple_of((core * depth + layer) * channels, channels)
        return remote(
            normed_buf.at[k], by_row.at[pl.ds(to, channels)], normed_send.at[k], normed_recv.at[k],
            tp_partner(k),
        )

    tap_0, tap_1, tap_2 = (column(taps_ref[i : i + 1, :]) for i in range(3))
    gain = column(head_ref[...])

    def convolve(k):
        j = (layer * 2 + core + k) & (devices - 1)
        wide = pl.ds(pl.multiple_of(j * chunk, chunk), chunk + HALO)
        gated = conv_buf[:, wide].astype(jnp.float32) * gate_in_buf[:, wide].astype(jnp.float32)
        docs = jnp.broadcast_to(docs_buf[:, wide], (8, chunk + HALO))
        lane = lax.broadcasted_iota(jnp.int32, docs.shape, 1)
        docs = jnp.where((j == 0) & (me == 0) & (lane < HALO), -1, docs)
        same_one = (pltpu.roll(docs, 1, 1) == docs).astype(jnp.float32)[:1, HALO:]
        same_two = (pltpu.roll(docs, 2, 1) == docs).astype(jnp.float32)[:1, HALO:]
        conv = (
            tap_2 * gated[:, HALO:]
            + tap_1 * (pltpu.roll(gated, 1, 1)[:, HALO:] * same_one)
            + tap_0 * (pltpu.roll(gated, 2, 1)[:, HALO:] * same_two)
        )
        own = pl.ds(pl.multiple_of(j * chunk, chunk), chunk)
        value = gate_out_buf[:, own].astype(jnp.float32) * conv
        scale = lax.rsqrt(jnp.mean(value * value, axis=0, keepdims=True) + norm_eps)
        normed_buf[k] = (value * scale * gain).astype(jnp.bfloat16)

    for load in loads[1:5]:
        load.wait()
    first_chunk = (devices - layer * 2 - core) & (devices - 1)

    @pl.loop(1, devices)
    def _(i):
        convolve((first_chunk + i) & (devices - 1))

    pl.semaphore_wait(barrier, len(greeted))
    start(halo)
    loads[0].wait()
    start(deep)

    half = resid_buf.shape[0] // BLOCKS
    slot = send_buf.shape[3]
    slots = PARTNERS * slot
    dy = ((ids_ref[...] >> 2) - (me >> 2)) & (SIDE - 1)
    dx = (ids_ref[...] - me) & (SIDE - 1)
    f_of = dx * (1 - core) + dy * core
    g_of = (dy * (1 - core) + dx * core + SIDE - 1) & (SIDE - 1)
    group = f_of * SIDE + g_of
    earlier = (
        lax.broadcasted_iota(jnp.int32, (half, half), 0) < lax.broadcasted_iota(jnp.int32, (half, half), 1)
    ).astype(jnp.bfloat16)
    for b in range(BLOCKS):
        counted = jnp.zeros((PARTNERS, 1), jnp.float32)
        marked = jnp.zeros((slots, half), jnp.float32)
        shares = jnp.zeros((slots, half), jnp.float32)
        for choice in range(2):
            mine = group[choice : choice + 1, b * half : (b + 1) * half]
            marks = (lax.broadcasted_iota(jnp.int32, (PARTNERS, half), 0) == mine).astype(jnp.float32)
            before = counted + jnp.dot(
                marks.astype(jnp.bfloat16), earlier, preferred_element_type=jnp.float32
            )
            place = mine.astype(jnp.float32) * slot + jnp.sum(marks * before, axis=0, keepdims=True)
            counted = counted + jnp.sum(marks, axis=1, keepdims=True)
            hit = lax.broadcasted_iota(jnp.int32, (slots, half), 0).astype(jnp.float32) == place
            marked = jnp.where(hit, 1.0, marked)
            shares = jnp.where(hit, share_ref[choice : choice + 1, b * half : (b + 1) * half], shares)
        table_ref[b] = marked.astype(jnp.bfloat16)
        by_position = shares.T
        high = by_position.astype(jnp.bfloat16)
        weight_hi[b] = high
        weight_lo[b] = (by_position - high.astype(jnp.float32)).astype(jnp.bfloat16)

    arrived(halo)
    convolve(first_chunk)

    def piece(f, g, c):
        return proj.at[c, place_at(c, f, g)]

    def pair_copy(f, g, c):
        at = (f & (SIDE - 1), g & (SIDE - 1))
        return remote(piece(f, g, c), piece(f, g, c), pair_send.at[at], pair_recv.at[at], {"tp_1": 1 - core})

    def row_copy(f):
        return remote(
            piece(0, 0, core), piece(0, 0, core), row_send.at[f - 1], row_recv.at[f - 1], partner(f, 0)
        )

    def plane_copy(f, g):
        return remote(
            piece(-f, 0, core), piece(-f, 0, core), plane_send.at[f, g - 1], plane_recv.at[f, g - 1],
            partner(0, g),
        )

    arrived(deep)
    start([row_copy(f) for f in (1, 3, 2)])
    start([plane_copy(0, g) for g in (1, 3, 2)])
    pair_copy(0, 0, core).start()

    @pl.loop(0, devices - 1)
    def _(i):
        normed_copy(devices // 2 + jnp.where((i & 1) == 1, -((i + 1) >> 1), i >> 1)).start()

    by_row[pl.ds(pl.multiple_of((core * depth + layer) * channels, channels), channels)] = normed_buf[0]
    for f in (1, 3, 2):
        row_copy(f).wait_recv()
        start([plane_copy(f, g) for g in (1, 3, 2)])
        pair_copy(-f, 0, core).start()
    loads[5].wait()
    squares[...] = jnp.zeros_like(squares)

    @pl.loop(1, devices)
    def _(k):
        normed_copy(k).wait_recv()

    turned[...] = by_row[...].T

    def ordered(i):
        return i ^ (i >> 1)

    for n in range(SIDE):
        if n:

            @pl.loop(0, SIDE)
            def _(i):
                plane_copy(ordered(i), ordered(n)).wait_recv()
                pair_copy(-ordered(i), -ordered(n), core).start()

        @pl.loop(0, 2 * n + 1)
        def _(m):
            f, g = ordered(jnp.minimum(m, n)), ordered(jnp.minimum(n, 2 * n - m))
            pair_copy(-g, -f, 1 - core).wait_recv()
            at = place_at(core, -f, -g)
            col = pl.ds(pl.multiple_of(at * LANES, LANES), LANES)
            mixed = jnp.dot(
                turned[:, : depth * channels], proj[0, at], preferred_element_type=jnp.float32
            ) + jnp.dot(turned[:, depth * channels :], proj[1, at], preferred_element_type=jnp.float32)
            value = resid_buf[:, col].astype(jnp.float32) + mixed
            stream_ref[:, col] = value
            squares[...] += value * value

    mean = jnp.sum(squares[...], axis=1, keepdims=True) / (PARTNERS * LANES)
    scale = lax.rsqrt(mean + norm_eps)
    step = 2 * LANES

    @pl.loop(0, PARTNERS * LANES // step)
    def _(i):
        col = pl.ds(pl.multiple_of(i * step, step), step)
        rows_ref[:, col] = (stream_ref[:, col] * scale * norm_ref[:, col]).astype(jnp.bfloat16)

    width = rows_ref.shape[1]
    cols = 512

    def pack(block, f):
        @pl.loop(0, width // cols)
        def _(c):
            col = pl.ds(pl.multiple_of(c * cols, cols), cols)
            packed = jnp.dot(
                table_ref[block, pl.ds(f * SIDE * slot, SIDE * slot)],
                rows_ref[pl.ds(block * half, half), col],
                preferred_element_type=jnp.float32,
            ).astype(jnp.bfloat16).reshape(SIDE, slot, cols)
            if f:
                send_buf[block, f, :, :, col] = packed
            else:
                there[block, pl.ds(0, SIDE), 0, :, col] = packed

    def experts(block, m):
        at = pl.ds(SIDE - 1 + m * 2, 2)
        inputs = there[block, at].reshape(slots // 2, width)
        gate = jnp.dot(inputs, gate_ref[...], preferred_element_type=jnp.float32)
        up = jnp.dot(inputs, up_ref[...], preferred_element_type=jnp.float32)
        hidden = (gate / (1.0 + jnp.exp(-gate)) * up).astype(jnp.bfloat16)
        result = jnp.dot(hidden, down_ref[...], preferred_element_type=jnp.float32)
        answers[block, at] = result.astype(jnp.bfloat16).reshape(2, SIDE, slot, width)

    def combine(block):
        @pl.loop(0, width // cols)
        def _(c):
            col = pl.ds(pl.multiple_of(c * cols, cols), cols)
            own = pl.ds(block * half, half)
            back = back_buf[block, :, :, :, col].reshape(slots, cols)
            total = (
                stream_ref[own, col]
                + jnp.dot(weight_hi[block], back, preferred_element_type=jnp.float32)
                + jnp.dot(weight_lo[block], back, preferred_element_type=jnp.float32)
            )
            out_ref[own, col] = total.astype(jnp.bfloat16)

    def ahead(i, b):
        return sems[2 * i].at[b], sems[2 * i + 1].at[b]

    every = pl.ds(0, SIDE)
    out_first = [
        copies_to(
            [send_buf.at[b, f] for f in others], [there.at[b, every, f] for f in others],
            *ahead(0, b), [partner(f, 0) for f in others],
        )
        for b in range(BLOCKS)
    ]
    out_second = [
        copies_to(
            [there.at[b, g - 1] for g in others], [there.at[b, SIDE - 1 + g] for g in others],
            *ahead(1, b), [partner(0, g) for g in others],
        )
        for b in range(BLOCKS)
    ]
    back_second = [
        copies_to(
            [answers.at[b, SIDE - 1 + g] for g in others], [answers.at[b, g - 1] for g in others],
            *ahead(2, b), [partner(0, SIDE - g) for g in others],
        )
        for b in range(BLOCKS)
    ]
    back_first = [
        copies_to(
            [answers.at[b, every, f] for f in others], [back_buf.at[b, f] for f in others],
            *ahead(3, b), [partner(SIDE - f, 0) for f in others],
        )
        for b in range(BLOCKS)
    ]
    own = [
        pltpu.make_async_copy(answers.at[b, every, 0], back_buf.at[b, 0], own_sems.at[b])
        for b in range(BLOCKS)
    ]

    pack(0, 2)
    pack(0, 1)
    out_first[0][1].start()
    pack(0, 3)
    out_first[0][0].start()
    pack(0, 0)
    out_first[0][2].start()
    arrived(out_first[0])
    start([out_second[0][i] for i in (1, 0, 2)])
    pack(1, 2)
    pack(1, 1)
    out_first[1][1].start()
    pack(1, 3)
    out_first[1][0].start()
    pack(1, 0)
    out_first[1][2].start()
    arrived(out_first[1])
    start([out_second[1][i] for i in (1, 0, 2)])
    for load in loads[6:]:
        load.wait()
    for b in range(BLOCKS):
        arrived(out_second[b][1:])
        experts(b, 1)
        start(back_second[b][1:])
        arrived(out_second[b][:1])
        experts(b, 0)
        start(back_second[b][:1])
    for b in range(BLOCKS):
        arrived(back_second[b])
        start([back_first[b][i] for i in (1, 0, 2)])
        own[b].start()
    for b in range(BLOCKS):
        arrived(back_first[b])
        own[b].wait()
        combine(b)

    @pl.loop(1, devices)
    def _(k):
        normed_copy(k).wait_send()

    @pl.loop(0, PARTNERS)
    def _(i):
        f, g = i & (SIDE - 1), i >> 2
        pair_copy(-f, -g, core).wait_send()

        @pl.when(g > 0)
        def _():
            plane_copy(f, g).wait_send()

    for copies in (halo, deep, [row_copy(f) for f in others], *out_first, *out_second, *back_second, *back_first):
        for copy in copies:
            copy.wait_send()


def layer_call(
    conv_in, in_gate, out_gate, docs, taps, head_gain, out_proj, resid, norm_gain,
    route_ids, route_weight, w_gate, w_up, w_down,
):
    count, width = resid.shape
    channels, length = conv_in.shape
    slot = max(2, count // 8)
    half = count // BLOCKS
    ff = w_gate.shape[1]
    depth = lax.axis_size("tp_0")
    devices = 2 * depth
    bf16 = jnp.bfloat16
    vmem = pl.BlockSpec(memory_space=pltpu.VMEM)
    hbm = pl.BlockSpec(memory_space=pl.ANY)
    square = pltpu.VMEM((BLOCKS, SIDE, SIDE, slot, width), bf16)
    longer = pltpu.VMEM((BLOCKS, 2 * SIDE - 1, SIDE, slot, width), bf16)
    dma = pltpu.SemaphoreType.DMA
    return pl.pallas_call(
        layer_kernel,
        out_shape=jax.ShapeDtypeStruct((count, width), bf16),
        in_specs=[vmem] * 5 + [hbm] * 9,
        out_specs=vmem,
        scratch_shapes=[
            pltpu.VMEM((channels, HALO + length), bf16),
            pltpu.VMEM((channels, HALO + length), bf16),
            pltpu.VMEM((channels, length), bf16),
            pltpu.VMEM((1, HALO + length), jnp.int32),
            pltpu.VMEM((count, width), bf16),
            pltpu.VMEM((devices, channels, length // devices), bf16),
            pltpu.VMEM((devices * channels, count), bf16),
            pltpu.VMEM((count, devices * channels), bf16),
            pltpu.VMEM((2, PARTNERS, depth * channels, width // PARTNERS), bf16),
            pltpu.VMEM((count, width), bf16),
            pltpu.VMEM((count, width), jnp.float32),
            pltpu.VMEM((count, LANES), jnp.float32),
            pltpu.VMEM((BLOCKS, PARTNERS * slot, half), bf16),
            pltpu.VMEM((BLOCKS, half, PARTNERS * slot), bf16),
            pltpu.VMEM((BLOCKS, half, PARTNERS * slot), bf16),
            square, longer, longer, square,
            pltpu.VMEM((width, ff), bf16),
            pltpu.VMEM((width, ff), bf16),
            pltpu.VMEM((ff, width), bf16),
            dma((9,)), dma((BLOCKS,)),
            dma((3,)), dma((3,)), dma((devices,)), dma((devices,)),
            dma((depth - 1,)), dma((depth - 1,)), dma((SIDE - 1,)), dma((SIDE - 1,)),
            dma((SIDE, SIDE - 1)), dma((SIDE, SIDE - 1)), dma((SIDE, SIDE)), dma((SIDE, SIDE)),
            *[dma((BLOCKS, SIDE - 1))] * 8,
        ],
        compiler_params=pltpu.CompilerParams(
            collective_id=1, has_side_effects=True, vmem_limit_bytes=60 * 1024 * 1024
        ),
        name="layer",
    )(
        taps, head_gain, norm_gain, route_ids, route_weight,
        conv_in, in_gate, out_gate, docs, out_proj, resid, w_gate, w_up, w_down,
    )


def body(
    conv_in,
    in_gate,
    out_gate,
    doc_ids,
    conv_taps,
    head_gain,
    out_proj,
    resid,
    norm_gain,
    route_ids,
    route_weight,
    w_gate,
    w_up,
    w_down,
):
    return layer_call(
        conv_in, in_gate, out_gate, doc_ids.reshape(1, -1), conv_taps.T, head_gain.reshape(1, -1),
        out_proj, resid, norm_gain.reshape(1, -1), route_ids.T, route_weight.T,
        w_gate[0], w_up[0], w_down[0],
    )


def solution(mesh):
    finer = Mesh(mesh.devices.reshape(mesh.shape["sp"], 8, 2), ("sp", "tp_0", "tp_1"))
    return jax.shard_map(
        body,
        mesh=finer,
        in_specs=(
            P(TP, "sp"),
            P(TP, "sp"),
            P(TP, "sp"),
            P("sp"),
            P(TP, None),
            P(TP),
            P(TP, None),
            P(SP_TP, None),
            P(),
            P(SP_TP, None),
            P(SP_TP, None),
            P("sp", None, None),
            P("sp", None, None),
            P("sp", None, None),
        ),
        out_specs=P(SP_TP, None),
        check_vma=False,
    )
```

```python
import jax
import jax.numpy as jnp
from jax import lax
from jax.experimental import pallas as pl
from jax.experimental.pallas import tpu as pltpu
from jax.sharding import Mesh
from jax.sharding import PartitionSpec as P

HEAD = 64
TP = ("tp_0", "tp_1")
LANES = 128
HALO = LANES
SP_TP = ("sp", "tp_0", "tp_1")
SIDE = 4
PARTNERS = SIDE * SIDE
BLOCKS = 2


norm_eps = 1e-06


def core_index():
    return lax.axis_index("tp_1")


def place_at(core, first, second):
    me = lax.axis_index("sp")
    step_y = core * first + (1 - core) * second
    step_x = (1 - core) * first + core * second
    y = ((me >> 2) + step_y) & (SIDE - 1)
    x = ((me & (SIDE - 1)) + step_x) & (SIDE - 1)
    return y * SIDE + x


def partner(first, second):
    return {"sp": place_at(core_index(), first, second)}


def tp_partner(steps):
    depth = lax.axis_size("tp_0")
    tp = (lax.axis_index("tp_0") * 2 + core_index() + steps) & (2 * depth - 1)
    return {"tp_0": tp >> 1, "tp_1": tp & 1}


def next_block(steps):
    return {"sp": (lax.axis_index("sp") + steps) & (PARTNERS - 1)}


def remote(source, target, send, recv, device):
    return pltpu.make_async_remote_copy(
        source, target, send, recv, device_id=device, device_id_type=pl.DeviceIdType.MESH
    )


def copies_to(sources, targets, send, recv, partners):
    return [
        remote(source, target, send.at[i], recv.at[i], device)
        for i, (source, target, device) in enumerate(zip(sources, targets, partners))
    ]


def start(copies):
    for copy in copies:
        copy.start()


def arrived(copies):
    for copy in copies:
        copy.wait_recv()


def layer_kernel(
    taps_ref, head_ref, norm_ref, ids_ref, share_ref,
    conv_hbm, gate_in_hbm, gate_out_hbm, docs_hbm, proj_hbm, resid_hbm,
    gate_hbm, up_hbm, down_hbm,
    out_ref,
    conv_buf, gate_in_buf, gate_out_buf, docs_buf, resid_buf, normed_buf, by_row, turned,
    proj, rows_ref, stream_ref, squares, table_ref, weight_hi, weight_lo,
    send_buf, there, answers, back_buf, gate_ref, up_ref, down_ref, load_sems, own_sems,
    halo_send, halo_recv, normed_send, normed_recv,
    deep_send, deep_recv, row_send, row_recv, plane_send, plane_recv, pair_send, pair_recv,
    *sems,
):
    me, core, layer = lax.axis_index("sp"), core_index(), lax.axis_index("tp_0")
    depth = lax.axis_size("tp_0")
    devices = 2 * depth
    channels, length = gate_out_buf.shape
    chunk = length // devices
    others = range(1, SIDE)
    barrier = pltpu.get_barrier_semaphore()
    greeted = [partner(step, 0) for step in others] + [partner(0, step) for step in others]
    greeted += [next_block(1), next_block(-1)] + [tp_partner(k) for k in range(1, devices)]
    for device in greeted:
        pl.semaphore_signal(barrier, inc=1, device_id=device, device_id_type=pl.DeviceIdType.MESH)

    body_at, halo_at = pl.ds(HALO, length), pl.ds(0, HALO)
    tail_at = pl.ds(length, HALO)
    own_shard = pl.ds(pl.multiple_of(layer * channels, channels), channels)
    own_cols = pl.ds(pl.multiple_of(me * LANES, LANES), LANES)
    pairs = (
        (proj_hbm.at[:, own_cols], proj.at[core, me, own_shard]),
        (conv_hbm, conv_buf.at[:, body_at]),
        (gate_in_hbm, gate_in_buf.at[:, body_at]),
        (docs_hbm, docs_buf.at[:, body_at]),
        (gate_out_hbm, gate_out_buf),
        (resid_hbm, resid_buf),
        (gate_hbm, gate_ref),
        (up_hbm, up_ref),
        (down_hbm, down_ref),
    )
    loads = [
        pltpu.make_async_copy(source, target, load_sems.at[i])
        for i, (source, target) in enumerate(pairs)
    ]
    start(loads)
    halo = [
        remote(buf.at[:, tail_at], buf.at[:, halo_at], halo_send.at[i], halo_recv.at[i], next_block(1))
        for i, buf in enumerate((conv_buf, gate_in_buf, docs_buf))
    ]
    deep = [
        remote(
            proj.at[core, me, own_shard], proj.at[core, me, own_shard],
            deep_send.at[k - 1], deep_recv.at[k - 1], tp_partner(2 * k),
        )
        for k in range(1, depth)
    ]
    def column(row):
        square = (row.shape[1], row.shape[1])
        diagonal = lax.broadcasted_iota(jnp.int32, square, 0) == lax.broadcasted_iota(jnp.int32, square, 1)
        return jnp.sum(jnp.where(diagonal, jnp.broadcast_to(row, square), 0.0), axis=1, keepdims=True)

    def normed_copy(k):
        to = pl.multiple_of((core * depth + layer) * channels, channels)
        return remote(
            normed_buf.at[k], by_row.at[pl.ds(to, channels)], normed_send.at[k], normed_recv.at[k],
            tp_partner(k),
        )

    tap_0, tap_1, tap_2 = (column(taps_ref[i : i + 1, :]) for i in range(3))
    gain = column(head_ref[...])

    def convolve(k):
        j = (layer * 2 + core + k) & (devices - 1)
        wide = pl.ds(pl.multiple_of(j * chunk, chunk), chunk + HALO)
        gated = conv_buf[:, wide].astype(jnp.float32) * gate_in_buf[:, wide].astype(jnp.float32)
        docs = jnp.broadcast_to(docs_buf[:, wide], (8, chunk + HALO))
        lane = lax.broadcasted_iota(jnp.int32, docs.shape, 1)
        docs = jnp.where((j == 0) & (me == 0) & (lane < HALO), -1, docs)
        same_one = (pltpu.roll(docs, 1, 1) == docs).astype(jnp.float32)[:1, HALO:]
        same_two = (pltpu.roll(docs, 2, 1) == docs).astype(jnp.float32)[:1, HALO:]
        conv = (
            tap_2 * gated[:, HALO:]
            + tap_1 * (pltpu.roll(gated, 1, 1)[:, HALO:] * same_one)
            + tap_0 * (pltpu.roll(gated, 2, 1)[:, HALO:] * same_two)
        )
        own = pl.ds(pl.multiple_of(j * chunk, chunk), chunk)
        value = gate_out_buf[:, own].astype(jnp.float32) * conv
        scale = lax.rsqrt(jnp.mean(value * value, axis=0, keepdims=True) + norm_eps)
        normed_buf[k] = (value * scale * gain).astype(jnp.bfloat16)

    for load in loads[1:5]:
        load.wait()
    first_chunk = (devices - layer * 2 - core) & (devices - 1)

    @pl.loop(1, devices)
    def _(i):
        convolve((first_chunk + i) & (devices - 1))

    pl.semaphore_wait(barrier, len(greeted))
    start(halo)
    loads[0].wait()
    start(deep)

    half = resid_buf.shape[0] // BLOCKS
    slot = send_buf.shape[3]
    slots = PARTNERS * slot
    dy = ((ids_ref[...] >> 2) - (me >> 2)) & (SIDE - 1)
    dx = (ids_ref[...] - me) & (SIDE - 1)
    f_of = dx * (1 - core) + dy * core
    g_of = (dy * (1 - core) + dx * core + SIDE - 1) & (SIDE - 1)
    group = f_of * SIDE + g_of
    earlier = (
        lax.broadcasted_iota(jnp.int32, (half, half), 0) < lax.broadcasted_iota(jnp.int32, (half, half), 1)
    ).astype(jnp.bfloat16)
    for b in range(BLOCKS):
        counted = jnp.zeros((PARTNERS, 1), jnp.float32)
        marked = jnp.zeros((slots, half), jnp.float32)
        shares = jnp.zeros((slots, half), jnp.float32)
        for choice in range(2):
            mine = group[choice : choice + 1, b * half : (b + 1) * half]
            marks = (lax.broadcasted_iota(jnp.int32, (PARTNERS, half), 0) == mine).astype(jnp.float32)
            before = counted + jnp.dot(
                marks.astype(jnp.bfloat16), earlier, preferred_element_type=jnp.float32
            )
            place = mine.astype(jnp.float32) * slot + jnp.sum(marks * before, axis=0, keepdims=True)
            counted = counted + jnp.sum(marks, axis=1, keepdims=True)
            hit = lax.broadcasted_iota(jnp.int32, (slots, half), 0).astype(jnp.float32) == place
            marked = jnp.where(hit, 1.0, marked)
            shares = jnp.where(hit, share_ref[choice : choice + 1, b * half : (b + 1) * half], shares)
        table_ref[b] = marked.astype(jnp.bfloat16)
        by_position = shares.T
        high = by_position.astype(jnp.bfloat16)
        weight_hi[b] = high
        weight_lo[b] = (by_position - high.astype(jnp.float32)).astype(jnp.bfloat16)

    arrived(halo)
    convolve(first_chunk)

    def piece(f, g, c):
        return proj.at[c, place_at(c, f, g)]

    def pair_copy(f, g, c):
        at = (f & (SIDE - 1), g & (SIDE - 1))
        return remote(piece(f, g, c), piece(f, g, c), pair_send.at[at], pair_recv.at[at], {"tp_1": 1 - core})

    def row_copy(f):
        return remote(
            piece(0, 0, core), piece(0, 0, core), row_send.at[f - 1], row_recv.at[f - 1], partner(f, 0)
        )

    def plane_copy(f, g):
        return remote(
            piece(-f, 0, core), piece(-f, 0, core), plane_send.at[f, g - 1], plane_recv.at[f, g - 1],
            partner(0, g),
        )

    arrived(deep)
    start([row_copy(f) for f in (2, 1, 3)])
    start([plane_copy(0, g) for g in (2, 1, 3)])
    pair_copy(0, 0, core).start()

    @pl.loop(0, devices - 1)
    def _(i):
        normed_copy(devices // 2 + jnp.where((i & 1) == 1, -((i + 1) >> 1), i >> 1)).start()

    by_row[pl.ds(pl.multiple_of((core * depth + layer) * channels, channels), channels)] = normed_buf[0]
    for f in (1, 3, 2):
        row_copy(f).wait_recv()
        start([plane_copy(f, g) for g in (2, 1, 3)])
        pair_copy(-f, 0, core).start()
    loads[5].wait()
    squares[...] = jnp.zeros_like(squares)

    @pl.loop(1, devices)
    def _(k):
        normed_copy(k).wait_recv()

    turned[...] = by_row[...].T

    def ordered(i):
        return i ^ (i >> 1)

    for n in range(SIDE):
        if n:

            @pl.loop(0, SIDE)
            def _(i):
                plane_copy(ordered(i), ordered(n)).wait_recv()
                pair_copy(-ordered(i), -ordered(n), core).start()

        @pl.loop(0, 2 * n + 1)
        def _(m):
            f, g = ordered(jnp.minimum(m, n)), ordered(jnp.minimum(n, 2 * n - m))
            pair_copy(-g, -f, 1 - core).wait_recv()
            at = place_at(core, -f, -g)
            col = pl.ds(pl.multiple_of(at * LANES, LANES), LANES)
            mixed = jnp.dot(
                turned[:, : depth * channels], proj[0, at], preferred_element_type=jnp.float32
            ) + jnp.dot(turned[:, depth * channels :], proj[1, at], preferred_element_type=jnp.float32)
            value = resid_buf[:, col].astype(jnp.float32) + mixed
            stream_ref[:, col] = value
            squares[...] += value * value

    mean = jnp.sum(squares[...], axis=1, keepdims=True) / (PARTNERS * LANES)
    scale = lax.rsqrt(mean + norm_eps)
    step = 2 * LANES

    @pl.loop(0, PARTNERS * LANES // step)
    def _(i):
        col = pl.ds(pl.multiple_of(i * step, step), step)
        rows_ref[:, col] = (stream_ref[:, col] * scale * norm_ref[:, col]).astype(jnp.bfloat16)

    width = rows_ref.shape[1]
    cols = 512

    def pack(block, f):
        @pl.loop(0, width // cols)
        def _(c):
            col = pl.ds(pl.multiple_of(c * cols, cols), cols)
            packed = jnp.dot(
                table_ref[block, pl.ds(f * SIDE * slot, SIDE * slot)],
                rows_ref[pl.ds(block * half, half), col],
                preferred_element_type=jnp.float32,
            ).astype(jnp.bfloat16).reshape(SIDE, slot, cols)
            if f:
                send_buf[block, f, :, :, col] = packed
            else:
                there[block, pl.ds(0, SIDE), 0, :, col] = packed

    def experts(block, m):
        at = pl.ds(SIDE - 1 + m * 2, 2)
        inputs = there[block, at].reshape(slots // 2, width)
        gate = jnp.dot(inputs, gate_ref[...], preferred_element_type=jnp.float32)
        up = jnp.dot(inputs, up_ref[...], preferred_element_type=jnp.float32)
        hidden = (gate / (1.0 + jnp.exp(-gate)) * up).astype(jnp.bfloat16)
        result = jnp.dot(hidden, down_ref[...], preferred_element_type=jnp.float32)
        answers[block, at] = result.astype(jnp.bfloat16).reshape(2, SIDE, slot, width)

    def combine(block):
        @pl.loop(0, width // cols)
        def _(c):
            col = pl.ds(pl.multiple_of(c * cols, cols), cols)
            own = pl.ds(block * half, half)
            back = back_buf[block, :, :, :, col].reshape(slots, cols)
            total = (
                stream_ref[own, col]
                + jnp.dot(weight_hi[block], back, preferred_element_type=jnp.float32)
                + jnp.dot(weight_lo[block], back, preferred_element_type=jnp.float32)
            )
            out_ref[own, col] = total.astype(jnp.bfloat16)

    def ahead(i, b):
        return sems[2 * i].at[b], sems[2 * i + 1].at[b]

    every = pl.ds(0, SIDE)
    out_first = [
        copies_to(
            [send_buf.at[b, f] for f in others], [there.at[b, every, f] for f in others],
            *ahead(0, b), [partner(f, 0) for f in others],
        )
        for b in range(BLOCKS)
    ]
    out_second = [
        copies_to(
            [there.at[b, g - 1] for g in others], [there.at[b, SIDE - 1 + g] for g in others],
            *ahead(1, b), [partner(0, g) for g in others],
        )
        for b in range(BLOCKS)
    ]
    back_second = [
        copies_to(
            [answers.at[b, SIDE - 1 + g] for g in others], [answers.at[b, g - 1] for g in others],
            *ahead(2, b), [partner(0, SIDE - g) for g in others],
        )
        for b in range(BLOCKS)
    ]
    back_first = [
        copies_to(
            [answers.at[b, every, f] for f in others], [back_buf.at[b, f] for f in others],
            *ahead(3, b), [partner(SIDE - f, 0) for f in others],
        )
        for b in range(BLOCKS)
    ]
    own = [
        pltpu.make_async_copy(answers.at[b, every, 0], back_buf.at[b, 0], own_sems.at[b])
        for b in range(BLOCKS)
    ]

    pack(0, 2)
    pack(0, 1)
    out_first[0][1].start()
    pack(0, 3)
    out_first[0][0].start()
    pack(0, 0)
    out_first[0][2].start()
    arrived(out_first[0])
    start([out_second[0][i] for i in (1, 0, 2)])
    pack(1, 2)
    pack(1, 1)
    out_first[1][1].start()
    pack(1, 3)
    out_first[1][0].start()
    pack(1, 0)
    out_first[1][2].start()
    arrived(out_first[1])
    start([out_second[1][i] for i in (1, 0, 2)])
    for load in loads[6:]:
        load.wait()
    arrived(out_second[0])
    experts(0, 1)
    experts(0, 0)
    start([back_second[0][i] for i in (1, 0, 2)])
    arrived(out_second[1])
    experts(1, 1)
    experts(1, 0)
    start([back_second[1][i] for i in (1, 0, 2)])
    for b in range(BLOCKS):
        arrived(back_second[b])
        start([back_first[b][i] for i in (1, 0, 2)])
        own[b].start()
    arrived(back_first[0])
    own[0].wait()
    combine(0)

    @pl.loop(1, devices)
    def _(k):
        normed_copy(k).wait_send()

    @pl.loop(0, PARTNERS)
    def _(i):
        f, g = i & (SIDE - 1), i >> 2
        pair_copy(-f, -g, core).wait_send()

        @pl.when(g > 0)
        def _():
            plane_copy(f, g).wait_send()

    for copies in (halo, deep, [row_copy(f) for f in others], *out_first, *out_second):
        for copy in copies:
            copy.wait_send()

    arrived(back_first[1])
    own[1].wait()
    combine(1)
    for copies in (*back_second, *back_first):
        for copy in copies:
            copy.wait_send()


def layer_call(
    conv_in, in_gate, out_gate, docs, taps, head_gain, out_proj, resid, norm_gain,
    route_ids, route_weight, w_gate, w_up, w_down,
):
    count, width = resid.shape
    channels, length = conv_in.shape
    slot = max(2, count // 8)
    half = count // BLOCKS
    ff = w_gate.shape[1]
    depth = lax.axis_size("tp_0")
    devices = 2 * depth
    bf16 = jnp.bfloat16
    vmem = pl.BlockSpec(memory_space=pltpu.VMEM)
    hbm = pl.BlockSpec(memory_space=pl.ANY)
    square = pltpu.VMEM((BLOCKS, SIDE, SIDE, slot, width), bf16)
    longer = pltpu.VMEM((BLOCKS, 2 * SIDE - 1, SIDE, slot, width), bf16)
    dma = pltpu.SemaphoreType.DMA
    return pl.pallas_call(
        layer_kernel,
        out_shape=jax.ShapeDtypeStruct((count, width), bf16),
        in_specs=[vmem] * 5 + [hbm] * 9,
        out_specs=vmem,
        scratch_shapes=[
            pltpu.VMEM((channels, HALO + length), bf16),
            pltpu.VMEM((channels, HALO + length), bf16),
            pltpu.VMEM((channels, length), bf16),
            pltpu.VMEM((1, HALO + length), jnp.int32),
            pltpu.VMEM((count, width), bf16),
            pltpu.VMEM((devices, channels, length // devices), bf16),
            pltpu.VMEM((devices * channels, count), bf16),
            pltpu.VMEM((count, devices * channels), bf16),
            pltpu.VMEM((2, PARTNERS, depth * channels, width // PARTNERS), bf16),
            pltpu.VMEM((count, width), bf16),
            pltpu.VMEM((count, width), jnp.float32),
            pltpu.VMEM((count, LANES), jnp.float32),
            pltpu.VMEM((BLOCKS, PARTNERS * slot, half), bf16),
            pltpu.VMEM((BLOCKS, half, PARTNERS * slot), bf16),
            pltpu.VMEM((BLOCKS, half, PARTNERS * slot), bf16),
            square, longer, longer, square,
            pltpu.VMEM((width, ff), bf16),
            pltpu.VMEM((width, ff), bf16),
            pltpu.VMEM((ff, width), bf16),
            dma((9,)), dma((BLOCKS,)),
            dma((3,)), dma((3,)), dma((devices,)), dma((devices,)),
            dma((depth - 1,)), dma((depth - 1,)), dma((SIDE - 1,)), dma((SIDE - 1,)),
            dma((SIDE, SIDE - 1)), dma((SIDE, SIDE - 1)), dma((SIDE, SIDE)), dma((SIDE, SIDE)),
            *[dma((BLOCKS, SIDE - 1))] * 8,
        ],
        compiler_params=pltpu.CompilerParams(
            collective_id=1, has_side_effects=True, vmem_limit_bytes=60 * 1024 * 1024
        ),
        name="layer",
    )(
        taps, head_gain, norm_gain, route_ids, route_weight,
        conv_in, in_gate, out_gate, docs, out_proj, resid, w_gate, w_up, w_down,
    )


def body(
    conv_in,
    in_gate,
    out_gate,
    doc_ids,
    conv_taps,
    head_gain,
    out_proj,
    resid,
    norm_gain,
    route_ids,
    route_weight,
    w_gate,
    w_up,
    w_down,
):
    return layer_call(
        conv_in, in_gate, out_gate, doc_ids.reshape(1, -1), conv_taps.T, head_gain.reshape(1, -1),
        out_proj, resid, norm_gain.reshape(1, -1), route_ids.T, route_weight.T,
        w_gate[0], w_up[0], w_down[0],
    )


def solution(mesh):
    finer = Mesh(mesh.devices.reshape(mesh.shape["sp"], 8, 2), ("sp", "tp_0", "tp_1"))
    return jax.shard_map(
        body,
        mesh=finer,
        in_specs=(
            P(TP, "sp"),
            P(TP, "sp"),
            P(TP, "sp"),
            P("sp"),
            P(TP, None),
            P(TP),
            P(TP, None),
            P(SP_TP, None),
            P(),
            P(SP_TP, None),
            P(SP_TP, None),
            P("sp", None, None),
            P("sp", None, None),
            P("sp", None, None),
        ),
        out_specs=P(SP_TP, None),
        check_vma=False,
    )
```
